32 devices in a mesh: ep: 4 (over y, x), tp: 8 (over z, core).
Axes of the slice: x: 2, y: 2, z: 4, core: 2. Of those that a mesh axis runs over, the one named last changes fastest.
Arguments:
- query_heads: bfloat16 [1024, 2048], P('ep', 'tp'), may hold values from -60 to 60
- key_heads: bfloat16 [1024, 2048], P('ep', 'tp'), may hold values from -40.5 to 40.5
- value_heads: bfloat16 [1024, 2048], P('ep', 'tp'), may hold values from -6 to 6
- diff_lambda: float32 [16], P('tp'), may hold values from 0.3 to 0.8
- sub_gain: float32 [128], replicated, may hold values from 0.1 to 1.9
- out_weight: bfloat16 [2048, 4096], P('tp'), may hold values from -0.125 to 0.125
- routed_input: bfloat16 [1024, 4096], P('ep', 'tp'), may hold values from -40 to 40
- routes: int32 [1024, 2], P('ep'), may hold values from 0 to 3, all different within a row; in each aligned block of 256 rows (0 to 255, 256 to 511, ...) at most 256 rows name the same one
- route_weights: float32 [1024, 2], P('ep'), may hold values from 0.3 to 1.5
- expert_gate: bfloat16 [4, 4096, 4096], P('ep', None, 'tp'), may hold values from -0.09375 to 0.09375
- expert_up: bfloat16 [4, 4096, 4096], P('ep', None, 'tp'), may hold values from -0.09375 to 0.09375
- expert_down: bfloat16 [4, 4096, 4096], P('ep', 'tp'), may hold values from -0.09375 to 0.09375
- shared_gate: bfloat16 [4096, 2048], P(None, 'tp'), may hold values from -0.09375 to 0.09375
- shared_up: bfloat16 [4096, 2048], P(None, 'tp'), may hold values from -0.09375 to 0.09375
- shared_down: bfloat16 [2048, 4096], P('tp'), may hold values from -0.125 to 0.125
Outputs:
- mixer_output: bfloat16 [1024, 4096], P('ep', 'tp')
- routed_output: bfloat16 [1024, 4096], P('ep', 'tp')
The draws below stay inside these ranges and needn't reach their ends.
Inputs may be any that keep to these rules, and one draw needn't show every extreme that they name: `routes`: each row names 2 different experts. In each aligned block of 256 rows no expert is named by more than 256 rows, a bound that some block reaches.
All inputs are finite; a program needn't handle non-finite values.
Results may differ from the reference program's by a relative error of at most 0.02.
Values may be sent and summed in bfloat16 or wider, within the bound.
No kernel may reach another device: no remote copies, remote signals or barrier semaphores. Data moves between devices by JAX's collectives and lax.ppermute only.
A program may use at most 128 MiB of HBM per device.

```python
import math
import jax
import jax.numpy as jnp
import numpy as np
from jax import lax

D = 4096
HEADS = 16
QK = 64
VD = 128
FF = 4096
FS = 2048
TOPK = 2
EXPERTS = 4
ROWS_B = 256
TOKENS_A = 1024
TOKENS_B = 1024
CAP = 256
N_EP = 4
N_TP = 8


def draw_query_heads(key, part):
    base_key = jax.random.fold_in(jax.random.fold_in(key, 11), 0)
    values = 1.3 * jnp.clip(jax.random.normal(base_key, (TOKENS_A, HEADS * 2 * QK), jnp.float32), -6.0, 6.0)
    return values.astype(jnp.bfloat16)


def draw_key_heads(key, part):
    base_key = jax.random.fold_in(jax.random.fold_in(key, 23), 0)
    values = 1.3 * jnp.clip(jax.random.normal(base_key, (TOKENS_A, HEADS * 2 * QK), jnp.float32), -6.0, 6.0)
    return values.astype(jnp.bfloat16)


def draw_routed_input(key, part):
    base_key, row_key = jax.random.split(jax.random.fold_in(key, 37))
    column_pos = jnp.arange(D, dtype=jnp.float32)[None, :] / D
    column_scale = 0.6 * jnp.exp(column_pos * jnp.log(3.0))
    row_scale = jnp.exp(jax.random.uniform(row_key, (TOKENS_B, 1), jnp.float32, jnp.log(0.7), jnp.log(1.4)))
    entries = jnp.clip(jax.random.normal(base_key, (TOKENS_B, D), jnp.float32), -6.0, 6.0)
    return (entries * column_scale * row_scale).astype(jnp.bfloat16)


def level_of(stream_key, shape, cuts, low, top_value):
    loudness = 1.0
    for axis_at, shards_of in cuts:
        draws = jax.random.uniform(jax.random.fold_in(jax.random.fold_in(stream_key, 6), axis_at), (shards_of,), jnp.float32, low / len(cuts), top_value / len(cuts))
        loudness = loudness * jnp.repeat(jnp.exp(draws), shape[axis_at] // shards_of).reshape((-1,) + (1,) * (len(shape) - 1 - axis_at))
    return loudness


def deal_out(rng, own, number, rows, amount, top, bound, lean):
    sequence = jax.random.permutation(rng, amount)
    heavy_load, common = shares(amount, rows * top, bound, lean, True), shares(amount, rows * top, bound, lean, False)
    places = jnp.arange(amount)

    def named(tallies, rotation):
        used = int((tallies > 0).sum())
        fixed = max(1, used // 4)
        passed = fixed + (places - fixed + rotation * (used - fixed)) % max(1, amount - fixed)
        return jnp.zeros((amount,), jnp.int32).at[sequence[jnp.where(places < fixed, places, passed)]].set(jnp.asarray(tallies, jnp.int32))

    tallies = jnp.where(number % 4 == 0, named(heavy_load, number // 4), named(common, number - number // 4 - 1))
    mixed = jax.random.permutation(jax.random.fold_in(own, 3), amount)
    giver, receiver = mixed[0:amount // 2 * 2:2], mixed[1:amount // 2 * 2:2]
    slack = jnp.minimum(tallies[giver] - 1, bound - tallies[receiver]) // 2
    slack = jnp.where((giver == sequence[0]) | (receiver == sequence[0]) | (tallies[receiver] == 0), 0, jnp.maximum(slack, 0))
    passed = jax.random.randint(jax.random.fold_in(own, 4), (amount // 2,), 0, 1 << 20) % (slack + 1)
    tallies = tallies.at[giver].add(-passed).at[receiver].add(passed)
    items = jnp.searchsorted(jnp.cumsum(tallies), jnp.arange(rows * top), side="right").astype(jnp.int32)
    grid = items.reshape(top, rows).T
    grid = grid[jax.random.permutation(jax.random.fold_in(own, 1), rows)]
    rotation = jax.random.randint(jax.random.fold_in(own, 2), (rows, 1), 0, top)
    return jnp.take_along_axis(grid, (jnp.arange(top)[None, :] + rotation) % top, axis=1)


def shares(amount, total, limit, skew, full):
    weights = [(1 << 20) // math.isqrt(rank ** skew) + 1 for rank in range(1, amount + 1)]
    largest = limit if full else min(limit, max(-(-total // amount), total * weights[0] // sum(weights)))
    least = 1 if total - largest >= amount - 1 else 0
    given, spare = [largest] + [least] * (amount - 1), total - largest - least * (amount - 1)
    while spare > 0:
        candidates = [i for i in range(1, amount) if given[i] < largest] or [i for i in range(1, amount) if given[i] < limit]
        pool, budget = sum([weights[i] for i in candidates]), spare
        for i in candidates:
            more = min(limit - given[i], max(1, budget * weights[i] // pool), spare)
            given[i] = given[i] + more
            spare = spare - more
    return np.array(given)


def normal_values(key, extent, deviation, bound, pieces=(), kind=jnp.bfloat16):
    drawn = jax.random.normal(key, extent, jnp.float32) * deviation
    if len(pieces) > 0:
        drawn = level_of(key, extent, pieces, -0.22, 0.18) * drawn
    return jnp.clip(drawn, min=-bound, max=bound).astype(kind)


def setup_inputs(seed: int = 0) -> dict:
    arg_keys = jax.random.split(jax.random.key(seed), 16)
    query_heads = draw_query_heads(jax.random.fold_in(arg_keys[15], 71), 0)
    key_heads = draw_key_heads(jax.random.fold_in(arg_keys[15], 71), 0)
    value_heads = normal_values(arg_keys[2], (TOKENS_A, HEADS * VD), 1.0, 6.0, ((0, 4), (1, 8)))
    diff_lambda = jnp.clip(0.3 + 0.5 * jax.random.uniform(arg_keys[3], (HEADS,), jnp.float32) ** level_of(arg_keys[3], (HEADS,), ((0, 8),), -0.2, 0.2), 0.3, 0.8)
    sub_gain = jnp.clip(1.0 + 0.18 * jax.random.normal(arg_keys[4], (VD,), jnp.float32), 0.1, 1.9)
    out_weight = normal_values(arg_keys[5], (HEADS * VD, D), (HEADS * VD) ** -0.5, 0.125, ((0, 8),))
    routed_input = draw_routed_input(jax.random.fold_in(arg_keys[15], 71), 0)
    routes_keys = jax.random.split(jax.random.fold_in(arg_keys[7], 1), TOKENS_B // ROWS_B)
    routes_turns = jax.random.permutation(jax.random.fold_in(arg_keys[7], 3), TOKENS_B // ROWS_B)
    routes = jax.vmap(lambda own, number: deal_out(jax.random.fold_in(arg_keys[7], 2), own, number, ROWS_B, EXPERTS, TOPK, CAP, 2))(routes_keys, routes_turns).reshape((TOKENS_B, TOPK))
    route_weights = jnp.clip(jnp.exp(math.log(1.5) - 1.60943787 * jax.random.uniform(arg_keys[8], (TOKENS_B, TOPK), jnp.float32) ** level_of(arg_keys[8], (TOKENS_B, TOPK), ((0, 4),), -0.2, 0.2)), 0.3, 1.5)
    expert_gate = normal_values(arg_keys[9], (EXPERTS, D, FF), D ** -0.5, 0.09375, ((0, 4), (2, 8)))
    expert_up = normal_values(arg_keys[10], (EXPERTS, D, FF), D ** -0.5, 0.09375, ((0, 4), (2, 8)))
    expert_down = normal_values(arg_keys[11], (EXPERTS, FF, D), FF ** -0.5, 0.09375, ((0, 4), (1, 8)))
    shared_gate = normal_values(arg_keys[12], (D, FS), D ** -0.5, 0.09375, ((1, 8),))
    shared_up = normal_values(arg_keys[13], (D, FS), D ** -0.5, 0.09375, ((1, 8),))
    shared_down = normal_values(arg_keys[14], (FS, D), FS ** -0.5, 0.125, ((0, 8),))
    return {"query_heads": query_heads, "key_heads": key_heads, "value_heads": value_heads, "diff_lambda": diff_lambda, "sub_gain": sub_gain, "out_weight": out_weight, "routed_input": routed_input, "routes": routes, "route_weights": route_weights, "expert_gate": expert_gate, "expert_up": expert_up, "expert_down": expert_down, "shared_gate": shared_gate, "shared_up": shared_up, "shared_down": shared_down}


ROPE_BASE = 10000.0
NORM_EPS = 1e-06
MASKED = -1e+30

def rotate(values, positions):
    half_width = values.shape[-1] // 2
    inverse_freq = ROPE_BASE ** (-jnp.arange(half_width, dtype=jnp.float32) / half_width)
    angles = positions.astype(jnp.float32)[:, None] * inverse_freq[None, :]
    angles = angles.reshape((angles.shape[0],) + (1,) * (values.ndim - 2) + (half_width,))
    cosine = jnp.cos(angles)
    sine_part = jnp.sin(angles)
    lower = values[..., :half_width]
    upper = values[..., half_width:]
    return jnp.concatenate([lower * cosine - upper * sine_part, upper * cosine + lower * sine_part], axis=-1)

def split_sum(left, right, groups):
    group_width = left.shape[1] // groups

    def add_group(summed, group_index):
        left_part = lax.dynamic_slice_in_dim(left, group_index * group_width, group_width, 1)
        right_part = lax.dynamic_slice_in_dim(right, group_index * group_width, group_width, 0)
        rounded = jnp.dot(left_part, right_part, preferred_element_type=jnp.float32).astype(jnp.bfloat16)
        rounded = lax.optimization_barrier(rounded)
        return (summed + rounded.astype(jnp.float32), None)
    start_sum = jnp.zeros((left.shape[0], right.shape[1]), jnp.float32)
    summed, _ = lax.scan(add_group, start_sum, jnp.arange(groups, dtype=jnp.int32))
    return summed

def attend_head(query_head, key_head, value_head, lambda_head, sub_gain):
    seq_len = query_head.shape[0]
    query_block = 512 if seq_len % 512 == 0 else seq_len
    score_scale = query_head.shape[-1] ** (-0.5)
    key_positions = jnp.arange(seq_len, dtype=jnp.int32)

    def one_block(block_index):
        block_start = block_index * query_block
        query_rows = lax.dynamic_slice_in_dim(query_head, block_start, query_block, 0)
        query_positions = block_start + jnp.arange(query_block, dtype=jnp.int32)
        visible = key_positions[None, :] <= query_positions[:, None]
        attended = []
        for which_map in range(2):
            scores = jnp.dot(query_rows[:, which_map], key_head[:, which_map].T, preferred_element_type=jnp.float32) * score_scale
            scores = jnp.where(visible, scores, MASKED)
            maxima = lax.optimization_barrier(jnp.max(scores, axis=1, keepdims=True))
            exp_weights = jnp.where(visible, jnp.exp(scores - maxima), 0.0)
            totals = lax.optimization_barrier(jnp.sum(exp_weights, axis=1, keepdims=True))
            weighted = jnp.dot(exp_weights.astype(jnp.bfloat16), value_head, preferred_element_type=jnp.float32)
            attended.append(weighted / totals)
        mixed_heads = attended[0] - lambda_head * attended[1]
        normed = mixed_heads * lax.rsqrt(lax.optimization_barrier(jnp.mean(mixed_heads * mixed_heads, axis=1, keepdims=True)) + NORM_EPS) * sub_gain
        return normed.astype(jnp.bfloat16)
    blocks = lax.map(one_block, jnp.arange(seq_len // query_block, dtype=jnp.int32))
    return blocks.reshape(seq_len, value_head.shape[1])

def expert_apply(token_rows, gate_weight, up_weight, down_weight):
    squares = lax.optimization_barrier(jnp.sum(jnp.square(token_rows.astype(jnp.float32)), axis=1, keepdims=True))
    factor = lax.rsqrt(squares / token_rows.shape[1] + NORM_EPS)
    gate_value = jnp.dot(token_rows, gate_weight, preferred_element_type=jnp.float32) * factor
    up_value = jnp.dot(token_rows, up_weight, preferred_element_type=jnp.float32) * factor
    hidden = (jax.nn.silu(gate_value) * up_value).astype(jnp.bfloat16)
    return split_sum(hidden, down_weight, N_TP)

def slot_table(routes, block_rows, capacity, experts):
    token_count, top_count = routes.shape
    block_total = token_count // block_rows
    grouped = routes.reshape(block_total, block_rows * top_count)
    onehot = (grouped[:, :, None] == jnp.arange(experts, dtype=jnp.int32)[None, None, :]).astype(jnp.int32)
    earlier = jnp.cumsum(onehot, axis=1) - onehot
    rank_within = lax.optimization_barrier(jnp.sum(earlier * onehot, axis=2))
    block_ids = jnp.arange(block_total, dtype=jnp.int32)[:, None]
    slot_index = grouped * (block_total * capacity) + block_ids * capacity + rank_within
    return slot_index.reshape(token_count * top_count)

def reference(query_heads, key_heads, value_heads, diff_lambda, sub_gain, out_weight, routed_input, routes, route_weights, expert_gate, expert_up, expert_down, shared_gate, shared_up, shared_down):
    seq_len = query_heads.shape[0]
    positions = jnp.arange(seq_len, dtype=jnp.int32)
    query_rot = rotate(query_heads.astype(jnp.float32).reshape(seq_len, HEADS, 2, QK), positions).astype(jnp.bfloat16)
    key_rot = rotate(key_heads.astype(jnp.float32).reshape(seq_len, HEADS, 2, QK), positions).astype(jnp.bfloat16)
    value_split = value_heads.reshape(seq_len, HEADS, VD)
    per_head = lax.map(lambda head_item: attend_head(head_item[0], head_item[1], head_item[2], head_item[3], sub_gain), (jnp.transpose(query_rot, (1, 0, 2, 3)), jnp.transpose(key_rot, (1, 0, 2, 3)), jnp.transpose(value_split, (1, 0, 2)), diff_lambda))
    heads_out = jnp.transpose(per_head, (1, 0, 2)).reshape(seq_len, HEADS * VD)
    mixer_output = split_sum(heads_out, out_weight, N_TP).astype(jnp.bfloat16)
    token_count = routed_input.shape[0]
    copies = token_count * TOPK
    slot_of_copy = slot_table(routes, ROWS_B, CAP, EXPERTS)
    per_expert = N_EP * CAP
    copy_token = jnp.arange(copies, dtype=jnp.int32) // TOPK
    token_table = jnp.zeros((EXPERTS * per_expert,), jnp.int32).at[slot_of_copy].set(copy_token)
    filled = jnp.zeros((EXPERTS * per_expert,), jnp.bfloat16).at[slot_of_copy].set(jnp.ones((copies,), jnp.bfloat16))
    gathered_rows = routed_input[token_table] * filled[:, None]
    expert_rows = gathered_rows.reshape(EXPERTS, per_expert, D)
    results = lax.map(lambda expert_item: expert_apply(expert_item[0], expert_item[1], expert_item[2], expert_item[3]), (expert_rows, expert_gate, expert_up, expert_down))
    results = results.astype(jnp.bfloat16).reshape(EXPERTS * per_expert, D)
    copy_results = results[slot_of_copy].reshape(token_count, TOPK, D)
    routed = lax.optimization_barrier(jnp.sum(copy_results.astype(jnp.float32) * route_weights[:, :, None], axis=1))
    shared_result = expert_apply(routed_input, shared_gate, shared_up, shared_down)
    routed_output = (routed + shared_result).astype(jnp.bfloat16)
    return (mixer_output, routed_output)
```

```python
import jax
import jax.numpy as jnp
from jax import lax
from jax.sharding import PartitionSpec as P

ROPE_BASE = 10000.0
NORM_EPS = 1e-06
MASKED = -1e30


def rotate(values, positions):
    half_width = values.shape[-1] // 2
    inverse_freq = ROPE_BASE ** (-jnp.arange(half_width, dtype=jnp.float32) / half_width)
    angles = positions.astype(jnp.float32)[:, None] * inverse_freq[None, :]
    angles = angles.reshape((angles.shape[0],) + (1,) * (values.ndim - 2) + (half_width,))
    cosine = jnp.cos(angles)
    sine_part = jnp.sin(angles)
    lower = values[..., :half_width]
    upper = values[..., half_width:]
    return jnp.concatenate(
        [lower * cosine - upper * sine_part, upper * cosine + lower * sine_part], axis=-1
    )


def mixer_terms(query_heads, key_heads, value_heads, diff_lambda, sub_gain, out_weight):
    row_count = query_heads.shape[0]
    local_heads = diff_lambda.shape[0]
    value_width = value_heads.shape[1] // local_heads
    key_width = query_heads.shape[1] // (2 * local_heads)
    score_scale = key_width ** (-0.5)
    offset = lax.axis_index("ep") * row_count
    positions = offset + jnp.arange(row_count, dtype=jnp.int32)
    last_row = offset + row_count - 1
    query_rot = rotate(
        query_heads.astype(jnp.float32).reshape(row_count, local_heads, 2, key_width), positions
    ).astype(jnp.bfloat16)
    queries = jnp.transpose(query_rot, (1, 2, 0, 3))
    key_rot = (
        rotate(
            key_heads.astype(jnp.float32).reshape(row_count, local_heads, 2, key_width), positions
        )
        .astype(jnp.bfloat16)
        .reshape(row_count, local_heads * 2 * key_width)
    )
    start_state = (
        jnp.full((local_heads, 2, row_count), MASKED, jnp.float32),
        jnp.zeros((local_heads, 2, row_count), jnp.float32),
        jnp.zeros((local_heads, 2, row_count, value_width), jnp.float32),
    )
    carried = start_state
    key_piece = lax.all_gather(key_rot, "ep", axis=0, tiled=True)
    value_piece = lax.all_gather(value_heads, "ep", axis=0, tiled=True)
    piece_rows = key_piece.shape[0]
    key_block = 512
    block_count = piece_rows // key_block
    key_blocks = key_piece.reshape(block_count, key_block, local_heads, 2, key_width)
    value_blocks = value_piece.reshape(block_count, key_block, local_heads, value_width)

    def block_step(running, block_item):
        key_rows, value_rows, block_index = block_item
        block_start = block_index * key_block

        def attend_block(partial_state):
            maxima, totals, weighted = partial_state
            key_positions = block_start + jnp.arange(key_block, dtype=jnp.int32)
            visible = key_positions[None, :] <= positions[:, None]
            scores = (
                jnp.einsum("hmqd,khmd->hmqk", queries, key_rows, preferred_element_type=jnp.float32)
                * score_scale
            )
            scores = jnp.where(visible, scores, MASKED)
            new_maxima = jnp.maximum(maxima, jnp.max(scores, axis=3))
            exp_weights = jnp.where(visible, jnp.exp(scores - new_maxima[..., None]), 0.0)
            shrink = jnp.exp(maxima - new_maxima)
            new_totals = totals * shrink + jnp.sum(exp_weights, axis=3)
            update = jnp.einsum(
                "hmqk,khw->hmqw",
                exp_weights.astype(jnp.bfloat16),
                value_rows,
                preferred_element_type=jnp.float32,
            )
            return (new_maxima, new_totals, weighted * shrink[..., None] + update)

        return (
            lax.cond(
                block_start <= last_row, attend_block, lambda partial_state: partial_state, running
            ),
            None,
        )

    carried, _ = lax.scan(
        block_step, carried, (key_blocks, value_blocks, jnp.arange(block_count, dtype=jnp.int32))
    )
    maxima, totals, weighted = carried
    attended = weighted / totals[..., None]
    mixed_heads = attended[:, 0] - diff_lambda[:, None, None] * attended[:, 1]
    normed = (
        mixed_heads
        * lax.rsqrt(jnp.mean(mixed_heads * mixed_heads, axis=2, keepdims=True) + NORM_EPS)
        * sub_gain
    )
    heads_out = jnp.transpose(normed.astype(jnp.bfloat16), (1, 0, 2)).reshape(
        row_count, local_heads * value_width
    )
    return jnp.dot(heads_out, out_weight, preferred_element_type=jnp.float32)


def expert_terms(
    routed_input, routes, expert_gate, expert_up, expert_down, shared_gate, shared_up, shared_down
):
    row_count, part_width = routed_input.shape
    top_count = routes.shape[1]
    local_experts = expert_gate.shape[0]
    groups = lax.axis_size("ep")
    experts = local_experts * groups
    capacity = 2 * row_count * top_count // experts
    copies = row_count * top_count
    flat_routes = routes.reshape(copies)
    onehot = (flat_routes[:, None] == jnp.arange(experts, dtype=jnp.int32)[None, :]).astype(
        jnp.int32
    )
    rank_within = jnp.sum((jnp.cumsum(onehot, axis=0) - onehot) * onehot, axis=1)
    slot_index = flat_routes * capacity + rank_within
    placer = (
        slot_index[:, None] == jnp.arange(experts * capacity, dtype=jnp.int32)[None, :]
    ).astype(jnp.bfloat16)
    token_slots = jnp.sum(placer.reshape(row_count, top_count, experts * capacity), axis=1)
    outgoing = jnp.dot(token_slots.T, routed_input, preferred_element_type=jnp.float32).astype(
        jnp.bfloat16
    )
    arrived = lax.all_to_all(
        outgoing.reshape(groups, local_experts * capacity, part_width),
        "ep",
        split_axis=0,
        concat_axis=0,
        tiled=True,
    )
    slot_count = groups * capacity
    slot_rows = jnp.transpose(
        arrived.reshape(groups, local_experts, capacity, part_width), (1, 0, 2, 3)
    ).reshape(local_experts, slot_count, part_width)
    slot_piece = lax.all_gather(slot_rows, "tp", axis=2, tiled=True)
    own_piece = lax.all_gather(routed_input[None], "tp", axis=2, tiled=True)
    own_rows = own_piece[0]
    gate_sum = jnp.einsum(
        "emc,ecf->emf", slot_piece, expert_gate, preferred_element_type=jnp.float32
    )
    up_sum = jnp.einsum("emc,ecf->emf", slot_piece, expert_up, preferred_element_type=jnp.float32)
    square_sum = jnp.sum(jnp.square(slot_piece.astype(jnp.float32)), axis=2)
    shared_gate_sum = jnp.dot(own_rows, shared_gate, preferred_element_type=jnp.float32)
    shared_up_sum = jnp.dot(own_rows, shared_up, preferred_element_type=jnp.float32)
    shared_square = jnp.sum(jnp.square(own_rows.astype(jnp.float32)), axis=1)
    full_width = expert_gate.shape[1]
    factor = lax.rsqrt(square_sum / full_width + NORM_EPS)[..., None]
    hidden = (jax.nn.silu(gate_sum * factor) * (up_sum * factor)).astype(jnp.bfloat16)
    shared_factor = lax.rsqrt(shared_square / full_width + NORM_EPS)[:, None]
    shared_hidden = (
        jax.nn.silu(shared_gate_sum * shared_factor) * (shared_up_sum * shared_factor)
    ).astype(jnp.bfloat16)
    shared_terms = jnp.dot(shared_hidden, shared_down, preferred_element_type=jnp.float32)
    routed_terms = jnp.einsum(
        "emf,efd->emd", hidden, expert_down, preferred_element_type=jnp.float32
    )
    routed_sum = lax.psum_scatter(
        routed_terms.astype(jnp.bfloat16), "tp", scatter_dimension=2, tiled=True
    ).astype(jnp.float32)
    return (routed_sum, shared_terms, placer)


def expert_finish(routed_sum, shared_sum, placer, route_weights):
    local_experts, slot_count, part_width = routed_sum.shape
    groups = lax.axis_size("ep")
    capacity = slot_count // groups
    leaving = jnp.transpose(
        routed_sum.astype(jnp.bfloat16).reshape(local_experts, groups, capacity, part_width),
        (1, 0, 2, 3),
    ).reshape(groups, local_experts * capacity, part_width)
    returned = lax.all_to_all(leaving, "ep", split_axis=0, concat_axis=0, tiled=True)
    copy_results = jnp.dot(
        placer,
        returned.reshape(groups * local_experts * capacity, part_width),
        preferred_element_type=jnp.float32,
    )
    row_count, top_count = route_weights.shape
    routed = jnp.sum(
        copy_results.reshape(row_count, top_count, part_width) * route_weights[:, :, None], axis=1
    )
    return (routed + shared_sum).astype(jnp.bfloat16)


def cores_swap():
    return [(t, t ^ 1) for t in range(lax.axis_size("tp"))]


def chip_shift(step):
    chips = lax.axis_size("tp") // 2
    return [
        (2 * z + c, 2 * ((z + step) % chips) + c) for z in range(chips) for c in range(2)
    ]


def flip(values, mask):
    return lax.ppermute(values, "ep", [(e, e ^ mask) for e in range(4)])


def gather_square(block):
    half = block.shape[0] // 2
    across = flip(block, 1)
    along = flip(block, 2)
    diag_low = flip(along[:half], 1)
    diag_high = flip(across[half:], 2)
    return [block, across, along, jnp.concatenate([diag_low, diag_high], axis=0)]


def scatter_square(blocks):
    half = blocks[0].shape[0] // 2
    low = blocks[3][:half].astype(jnp.bfloat16)
    high = blocks[3][half:].astype(jnp.bfloat16)
    from_across = flip(low, 1)
    from_along = flip(high, 2)
    across = jnp.concatenate([blocks[1][:half], blocks[1][half:] + from_along], axis=0)
    along = jnp.concatenate([blocks[2][:half] + from_across, blocks[2][half:]], axis=0)
    got_across = flip(across.astype(jnp.bfloat16), 1)
    got_along = flip(along.astype(jnp.bfloat16), 2)
    return blocks[0] + got_across.astype(jnp.float32) + got_along.astype(jnp.float32)


def dense_mixer(query_heads, key_heads, value_heads, diff_lambda, sub_gain, out_weight):
    row_count = query_heads.shape[0]
    local_heads = diff_lambda.shape[0]
    value_width = value_heads.shape[1] // local_heads
    key_width = query_heads.shape[1] // (2 * local_heads)
    score_scale = key_width ** (-0.5)
    index = lax.axis_index("ep")
    rows = jnp.arange(row_count, dtype=jnp.int32)
    positions = index * row_count + rows

    def turned(values):
        return rotate(
            values.astype(jnp.float32).reshape(row_count, local_heads, 2, key_width), positions
        ).astype(jnp.bfloat16)

    key_rot = turned(key_heads).reshape(row_count, local_heads * 2 * key_width)
    pieces = gather_square(jnp.concatenate([key_rot, value_heads], axis=1))
    queries = turned(query_heads)
    key_value = jnp.concatenate(pieces, axis=0)
    total_rows = key_value.shape[0]
    key_positions = jnp.concatenate([(index ^ j) * row_count + rows for j in range(4)])
    visible = key_positions[None, :] <= positions[:, None]
    split = local_heads * 2 * key_width
    keys = key_value[:, :split].reshape(total_rows, local_heads, 2, key_width)
    values = key_value[:, split:].reshape(total_rows, local_heads, value_width)
    scores = (
        jnp.einsum("qhmd,khmd->hmqk", queries, keys, preferred_element_type=jnp.float32)
        * score_scale
    )
    scores = jnp.where(visible, scores, MASKED)
    maxima = jnp.max(scores, axis=3, keepdims=True)
    exp_weights = jnp.exp(scores - maxima)
    totals = jnp.sum(exp_weights, axis=3, keepdims=True)
    weighted = jnp.einsum(
        "hmqk,khw->hmqw",
        exp_weights.astype(jnp.bfloat16),
        values,
        preferred_element_type=jnp.float32,
    )
    attended = weighted / totals
    mixed_heads = attended[:, 0] - diff_lambda[:, None, None] * attended[:, 1]
    normed = (
        mixed_heads
        * lax.rsqrt(jnp.mean(mixed_heads * mixed_heads, axis=2, keepdims=True) + NORM_EPS)
        * sub_gain
    )
    heads_out = jnp.transpose(normed.astype(jnp.bfloat16), (1, 0, 2)).reshape(
        row_count, local_heads * value_width
    )
    chips = lax.axis_size("tp") // 2
    place = lax.axis_index("tp")
    core = place % 2
    chip = place // 2
    partial = jnp.dot(heads_out, out_weight, preferred_element_type=jnp.float32).astype(
        jnp.bfloat16
    )
    width = partial.shape[1] // (2 * chips)
    parts = partial.reshape(row_count, chips, 2, width)
    mine = lax.dynamic_index_in_dim(parts, core, 2, keepdims=False)
    other = lax.dynamic_index_in_dim(parts, 1 - core, 2, keepdims=False)
    pair = mine.astype(jnp.float32) + lax.ppermute(other, "tp", cores_swap()).astype(jnp.float32)
    summed = lax.dynamic_index_in_dim(pair, chip, 1, keepdims=False)
    pair = pair.astype(jnp.bfloat16)
    for step in range(1, chips):
        leaving = lax.dynamic_index_in_dim(pair, (chip + step) % chips, 1, keepdims=False)
        summed = summed + lax.ppermute(leaving, "tp", chip_shift(step)).astype(jnp.float32)
    return summed.astype(jnp.bfloat16)


def dense_experts(
    routed_input,
    routes,
    route_weights,
    expert_gate,
    expert_up,
    expert_down,
    shared_gate,
    shared_up,
    shared_down,
):
    row_count, width = routed_input.shape
    chips = lax.axis_size("tp") // 2
    place = lax.axis_index("tp")
    core = place % 2
    chip = place // 2
    index = lax.axis_index("ep")
    full_width = expert_gate.shape[1]

    def weight_for(expert):
        return jnp.sum(jnp.where(routes == expert, route_weights, 0.0), axis=1)[None, :]

    combine = [weight_for(index)] + [flip(weight_for(index ^ j), j) for j in range(1, 4)]
    combine = jnp.concatenate(combine, axis=1).reshape(4 * row_count, 1)

    order = [0] + [k for k in (1, 3, 2) if k < chips]
    chip_blocks = [
        routed_input if k == 0 else lax.ppermute(routed_input, "tp", chip_shift(-k))
        for k in order
    ]

    def rows_of(weight, slot):
        return lax.dynamic_slice_in_dim(weight, slot * width, width, 0)

    def columns_of(weight, slot):
        return lax.dynamic_slice_in_dim(weight, slot * width, width, 1)

    def dot(left, right):
        return jnp.dot(left, right, preferred_element_type=jnp.float32)

    sums = [0.0, 0.0, 0.0, 0.0, 0.0]
    for k, block in zip(order, chip_blocks):
        held = jnp.concatenate(gather_square(block), axis=0)
        swapped = lax.ppermute(held, "tp", cores_swap())
        slot = ((chip + k) % chips) * 2
        for values, at in ((held, slot + core), (swapped, slot + 1 - core)):
            sums[0] = sums[0] + dot(values, rows_of(expert_gate[0], at))
            sums[1] = sums[1] + dot(values, rows_of(expert_up[0], at))
            sums[2] = sums[2] + dot(values[:row_count], rows_of(shared_gate, at))
            sums[3] = sums[3] + dot(values[:row_count], rows_of(shared_up, at))
            sums[4] = sums[4] + jnp.sum(
                jnp.square(values.astype(jnp.float32)), axis=1, keepdims=True
            )
    factor = lax.rsqrt(sums[4] / full_width + NORM_EPS)
    hidden = (jax.nn.silu(sums[0] * factor) * (sums[1] * factor) * combine).astype(jnp.bfloat16)
    own_factor = factor[:row_count]
    shared_hidden = (
        jax.nn.silu(sums[2] * own_factor) * (sums[3] * own_factor)
    ).astype(jnp.bfloat16)

    def partial(slot):
        down = columns_of(expert_down[0], slot)
        first = dot(hidden[:row_count], down) + dot(shared_hidden, columns_of(shared_down, slot))
        return first, dot(hidden[row_count:], down)

    total = 0.0
    for k in [k for k in (2, 1, 3) if k < chips] + [0]:
        slot = ((chip + k) % chips) * 2
        first, rest = partial(slot + 1 - core)
        leaving = jnp.concatenate(
            [first.astype(jnp.bfloat16), rest.astype(jnp.bfloat16)], axis=0
        )
        arrived = lax.ppermute(leaving, "tp", cores_swap()).astype(jnp.float32)
        first, rest = partial(slot + core)
        blocks = [first + arrived[:row_count]] + [
            rest[j * row_count : (j + 1) * row_count]
            + arrived[(j + 1) * row_count : (j + 2) * row_count]
            for j in range(3)
        ]
        result = scatter_square(blocks)
        if k:
            result = lax.ppermute(result.astype(jnp.bfloat16), "tp", chip_shift(k))
        total = total + result.astype(jnp.float32)
    return total.astype(jnp.bfloat16)


def body(
    query_heads,
    key_heads,
    value_heads,
    diff_lambda,
    sub_gain,
    out_weight,
    routed_input,
    routes,
    route_weights,
    expert_gate,
    expert_up,
    expert_down,
    shared_gate,
    shared_up,
    shared_down,
):
    groups = lax.axis_size("ep")
    local_experts = expert_gate.shape[0]
    capacity = 2 * routed_input.shape[0] * routes.shape[1] // (local_experts * groups)
    if (
        groups == 4
        and local_experts == 1
        and lax.axis_size("tp") in (4, 8)
        and capacity >= routed_input.shape[0]
    ):
        return (
            dense_mixer(query_heads, key_heads, value_heads, diff_lambda, sub_gain, out_weight),
            dense_experts(
                routed_input,
                routes,
                route_weights,
                expert_gate,
                expert_up,
                expert_down,
                shared_gate,
                shared_up,
                shared_down,
            ),
        )
    mixer_partial = mixer_terms(
        query_heads, key_heads, value_heads, diff_lambda, sub_gain, out_weight
    )
    routed_sum, shared_terms, placer = expert_terms(
        routed_input,
        routes,
        expert_gate,
        expert_up,
        expert_down,
        shared_gate,
        shared_up,
        shared_down,
    )
    mixer_sum, shared_sum = (
        lax.psum_scatter(
            mixer_partial.astype(jnp.bfloat16), "tp", scatter_dimension=1, tiled=True
        ).astype(jnp.float32),
        lax.psum_scatter(
            shared_terms.astype(jnp.bfloat16), "tp", scatter_dimension=1, tiled=True
        ).astype(jnp.float32),
    )
    return (
        mixer_sum.astype(jnp.bfloat16),
        expert_finish(routed_sum, shared_sum, placer, route_weights),
    )


def solution(mesh):
    placed = (
        P("ep", "tp"),
        P("ep", "tp"),
        P("ep", "tp"),
        P("tp"),
        P(),
        P("tp", None),
        P("ep", "tp"),
        P("ep", None),
        P("ep", None),
        P("ep", None, "tp"),
        P("ep", None, "tp"),
        P("ep", "tp", None),
        P(None, "tp"),
        P(None, "tp"),
        P("tp", None),
    )
    return jax.shard_map(
        body, mesh=mesh, in_specs=placed, out_specs=(P("ep", "tp"), P("ep", "tp")), check_vma=False
    )
```

```python
import jax
import jax.numpy as jnp
from jax import lax
from jax.sharding import PartitionSpec as P

ROPE_BASE = 10000.0
NORM_EPS = 1e-06
MASKED = -1e30


def rotate(values, positions):
    half_width = values.shape[-1] // 2
    inverse_freq = ROPE_BASE ** (-jnp.arange(half_width, dtype=jnp.float32) / half_width)
    angles = positions.astype(jnp.float32)[:, None] * inverse_freq[None, :]
    angles = angles.reshape((angles.shape[0],) + (1,) * (values.ndim - 2) + (half_width,))
    cosine = jnp.cos(angles)
    sine_part = jnp.sin(angles)
    lower = values[..., :half_width]
    upper = values[..., half_width:]
    return jnp.concatenate(
        [lower * cosine - upper * sine_part, upper * cosine + lower * sine_part], axis=-1
    )


def mixer_terms(query_heads, key_heads, value_heads, diff_lambda, sub_gain, out_weight):
    row_count = query_heads.shape[0]
    local_heads = diff_lambda.shape[0]
    value_width = value_heads.shape[1] // local_heads
    key_width = query_heads.shape[1] // (2 * local_heads)
    score_scale = key_width ** (-0.5)
    offset = lax.axis_index("ep") * row_count
    positions = offset + jnp.arange(row_count, dtype=jnp.int32)
    last_row = offset + row_count - 1
    query_rot = rotate(
        query_heads.astype(jnp.float32).reshape(row_count, local_heads, 2, key_width), positions
    ).astype(jnp.bfloat16)
    queries = jnp.transpose(query_rot, (1, 2, 0, 3))
    key_rot = (
        rotate(
            key_heads.astype(jnp.float32).reshape(row_count, local_heads, 2, key_width), positions
        )
        .astype(jnp.bfloat16)
        .reshape(row_count, local_heads * 2 * key_width)
    )
    start_state = (
        jnp.full((local_heads, 2, row_count), MASKED, jnp.float32),
        jnp.zeros((local_heads, 2, row_count), jnp.float32),
        jnp.zeros((local_heads, 2, row_count, value_width), jnp.float32),
    )
    carried = start_state
    key_piece = lax.all_gather(key_rot, "ep", axis=0, tiled=True)
    value_piece = lax.all_gather(value_heads, "ep", axis=0, tiled=True)
    piece_rows = key_piece.shape[0]
    key_block = 512
    block_count = piece_rows // key_block
    key_blocks = key_piece.reshape(block_count, key_block, local_heads, 2, key_width)
    value_blocks = value_piece.reshape(block_count, key_block, local_heads, value_width)

    def block_step(running, block_item):
        key_rows, value_rows, block_index = block_item
        block_start = block_index * key_block

        def attend_block(partial_state):
            maxima, totals, weighted = partial_state
            key_positions = block_start + jnp.arange(key_block, dtype=jnp.int32)
            visible = key_positions[None, :] <= positions[:, None]
            scores = (
                jnp.einsum("hmqd,khmd->hmqk", queries, key_rows, preferred_element_type=jnp.float32)
                * score_scale
            )
            scores = jnp.where(visible, scores, MASKED)
            new_maxima = jnp.maximum(maxima, jnp.max(scores, axis=3))
            exp_weights = jnp.where(visible, jnp.exp(scores - new_maxima[..., None]), 0.0)
            shrink = jnp.exp(maxima - new_maxima)
            new_totals = totals * shrink + jnp.sum(exp_weights, axis=3)
            update = jnp.einsum(
                "hmqk,khw->hmqw",
                exp_weights.astype(jnp.bfloat16),
                value_rows,
                preferred_element_type=jnp.float32,
            )
            return (new_maxima, new_totals, weighted * shrink[..., None] + update)

        return (
            lax.cond(
                block_start <= last_row, attend_block, lambda partial_state: partial_state, running
            ),
            None,
        )

    carried, _ = lax.scan(
        block_step, carried, (key_blocks, value_blocks, jnp.arange(block_count, dtype=jnp.int32))
    )
    maxima, totals, weighted = carried
    attended = weighted / totals[..., None]
    mixed_heads = attended[:, 0] - diff_lambda[:, None, None] * attended[:, 1]
    normed = (
        mixed_heads
        * lax.rsqrt(jnp.mean(mixed_heads * mixed_heads, axis=2, keepdims=True) + NORM_EPS)
        * sub_gain
    )
    heads_out = jnp.transpose(normed.astype(jnp.bfloat16), (1, 0, 2)).reshape(
        row_count, local_heads * value_width
    )
    return jnp.dot(heads_out, out_weight, preferred_element_type=jnp.float32)


def expert_terms(
    routed_input, routes, expert_gate, expert_up, expert_down, shared_gate, shared_up, shared_down
):
    row_count, part_width = routed_input.shape
    top_count = routes.shape[1]
    local_experts = expert_gate.shape[0]
    groups = lax.axis_size("ep")
    experts = local_experts * groups
    capacity = 2 * row_count * top_count // experts
    copies = row_count * top_count
    flat_routes = routes.reshape(copies)
    onehot = (flat_routes[:, None] == jnp.arange(experts, dtype=jnp.int32)[None, :]).astype(
        jnp.int32
    )
    rank_within = jnp.sum((jnp.cumsum(onehot, axis=0) - onehot) * onehot, axis=1)
    slot_index = flat_routes * capacity + rank_within
    placer = (
        slot_index[:, None] == jnp.arange(experts * capacity, dtype=jnp.int32)[None, :]
    ).astype(jnp.bfloat16)
    token_slots = jnp.sum(placer.reshape(row_count, top_count, experts * capacity), axis=1)
    outgoing = jnp.dot(token_slots.T, routed_input, preferred_element_type=jnp.float32).astype(
        jnp.bfloat16
    )
    arrived = lax.all_to_all(
        outgoing.reshape(groups, local_experts * capacity, part_width),
        "ep",
        split_axis=0,
        concat_axis=0,
        tiled=True,
    )
    slot_count = groups * capacity
    slot_rows = jnp.transpose(
        arrived.reshape(groups, local_experts, capacity, part_width), (1, 0, 2, 3)
    ).reshape(local_experts, slot_count, part_width)
    slot_piece = lax.all_gather(slot_rows, "tp", axis=2, tiled=True)
    own_piece = lax.all_gather(routed_input[None], "tp", axis=2, tiled=True)
    own_rows = own_piece[0]
    gate_sum = jnp.einsum(
        "emc,ecf->emf", slot_piece, expert_gate, preferred_element_type=jnp.float32
    )
    up_sum = jnp.einsum("emc,ecf->emf", slot_piece, expert_up, preferred_element_type=jnp.float32)
    square_sum = jnp.sum(jnp.square(slot_piece.astype(jnp.float32)), axis=2)
    shared_gate_sum = jnp.dot(own_rows, shared_gate, preferred_element_type=jnp.float32)
    shared_up_sum = jnp.dot(own_rows, shared_up, preferred_element_type=jnp.float32)
    shared_square = jnp.sum(jnp.square(own_rows.astype(jnp.float32)), axis=1)
    full_width = expert_gate.shape[1]
    factor = lax.rsqrt(square_sum / full_width + NORM_EPS)[..., None]
    hidden = (jax.nn.silu(gate_sum * factor) * (up_sum * factor)).astype(jnp.bfloat16)
    shared_factor = lax.rsqrt(shared_square / full_width + NORM_EPS)[:, None]
    shared_hidden = (
        jax.nn.silu(shared_gate_sum * shared_factor) * (shared_up_sum * shared_factor)
    ).astype(jnp.bfloat16)
    shared_terms = jnp.dot(shared_hidden, shared_down, preferred_element_type=jnp.float32)
    routed_terms = jnp.einsum(
        "emf,efd->emd", hidden, expert_down, preferred_element_type=jnp.float32
    )
    routed_sum = lax.psum_scatter(
        routed_terms.astype(jnp.bfloat16), "tp", scatter_dimension=2, tiled=True
    ).astype(jnp.float32)
    return (routed_sum, shared_terms, placer)


def expert_finish(routed_sum, shared_sum, placer, route_weights):
    local_experts, slot_count, part_width = routed_sum.shape
    groups = lax.axis_size("ep")
    capacity = slot_count // groups
    leaving = jnp.transpose(
        routed_sum.astype(jnp.bfloat16).reshape(local_experts, groups, capacity, part_width),
        (1, 0, 2, 3),
    ).reshape(groups, local_experts * capacity, part_width)
    returned = lax.all_to_all(leaving, "ep", split_axis=0, concat_axis=0, tiled=True)
    copy_results = jnp.dot(
        placer,
        returned.reshape(groups * local_experts * capacity, part_width),
        preferred_element_type=jnp.float32,
    )
    row_count, top_count = route_weights.shape
    routed = jnp.sum(
        copy_results.reshape(row_count, top_count, part_width) * route_weights[:, :, None], axis=1
    )
    return (routed + shared_sum).astype(jnp.bfloat16)


def cores_swap():
    return [(t, t ^ 1) for t in range(lax.axis_size("tp"))]


def chip_shift(step):
    chips = lax.axis_size("tp") // 2
    return [
        (2 * z + c, 2 * ((z + step) % chips) + c) for z in range(chips) for c in range(2)
    ]


def flip(values, mask):
    return lax.ppermute(values, "ep", [(e, e ^ mask) for e in range(4)])


def gather_square(block, relay):
    across = flip(block, 1)
    along = flip(block, 2)
    diag = flip(along, 1) if relay == 1 else flip(across, 2)
    return [block, across, along, diag]


def scatter_square(blocks, relay):
    passed = flip(blocks[3].astype(jnp.bfloat16), relay).astype(jnp.float32)
    across, along = blocks[1], blocks[2]
    if relay == 1:
        along = along + passed
    else:
        across = across + passed
    got_across = flip(across.astype(jnp.bfloat16), 1)
    got_along = flip(along.astype(jnp.bfloat16), 2)
    return blocks[0] + got_across.astype(jnp.float32) + got_along.astype(jnp.float32)


def dense_mixer(query_heads, key_heads, value_heads, diff_lambda, sub_gain, out_weight):
    row_count = query_heads.shape[0]
    local_heads = diff_lambda.shape[0]
    value_width = value_heads.shape[1] // local_heads
    key_width = query_heads.shape[1] // (2 * local_heads)
    score_scale = key_width ** (-0.5)
    index = lax.axis_index("ep")
    rows = jnp.arange(row_count, dtype=jnp.int32)
    positions = index * row_count + rows

    def turned(values):
        return rotate(
            values.astype(jnp.float32).reshape(row_count, local_heads, 2, key_width), positions
        ).astype(jnp.bfloat16)

    key_rot = turned(key_heads).reshape(row_count, local_heads * 2 * key_width)
    pieces = gather_square(jnp.concatenate([key_rot, value_heads], axis=1), 1)
    queries = turned(query_heads)
    key_value = jnp.concatenate(pieces, axis=0)
    total_rows = key_value.shape[0]
    key_positions = jnp.concatenate([(index ^ j) * row_count + rows for j in range(4)])
    visible = key_positions[None, :] <= positions[:, None]
    split = local_heads * 2 * key_width
    keys = key_value[:, :split].reshape(total_rows, local_heads, 2, key_width)
    values = key_value[:, split:].reshape(total_rows, local_heads, value_width)
    scores = (
        jnp.einsum("qhmd,khmd->hmqk", queries, keys, preferred_element_type=jnp.float32)
        * score_scale
    )
    scores = jnp.where(visible, scores, MASKED)
    maxima = jnp.max(scores, axis=3, keepdims=True)
    exp_weights = jnp.exp(scores - maxima)
    totals = jnp.sum(exp_weights, axis=3, keepdims=True)
    weighted = jnp.einsum(
        "hmqk,khw->hmqw",
        exp_weights.astype(jnp.bfloat16),
        values,
        preferred_element_type=jnp.float32,
    )
    attended = weighted / totals
    mixed_heads = attended[:, 0] - diff_lambda[:, None, None] * attended[:, 1]
    normed = (
        mixed_heads
        * lax.rsqrt(jnp.mean(mixed_heads * mixed_heads, axis=2, keepdims=True) + NORM_EPS)
        * sub_gain
    )
    heads_out = jnp.transpose(normed.astype(jnp.bfloat16), (1, 0, 2)).reshape(
        row_count, local_heads * value_width
    )
    chips = lax.axis_size("tp") // 2
    place = lax.axis_index("tp")
    core = place % 2
    chip = place // 2
    width = out_weight.shape[1] // (2 * chips)

    def part(slot):
        return jnp.dot(
            heads_out,
            lax.dynamic_slice_in_dim(out_weight, slot * width, width, 1),
            preferred_element_type=jnp.float32,
        )

    slots = [((chip + step) % chips) * 2 for step in range(chips)]
    leaving = jnp.concatenate(
        [part(slot + 1 - core).astype(jnp.bfloat16) for slot in slots], axis=0
    )
    arrived = lax.ppermute(leaving, "tp", cores_swap())
    summed = 0.0
    for step in list(range(1, chips)) + [0]:
        pair = part(slots[step] + core) + arrived[
            step * row_count : (step + 1) * row_count
        ].astype(jnp.float32)
        if step:
            pair = lax.ppermute(pair.astype(jnp.bfloat16), "tp", chip_shift(step))
        summed = summed + pair.astype(jnp.float32)
    return summed.astype(jnp.bfloat16)


def dense_experts(
    routed_input,
    routes,
    route_weights,
    expert_gate,
    expert_up,
    expert_down,
    shared_gate,
    shared_up,
    shared_down,
):
    row_count, width = routed_input.shape
    chips = lax.axis_size("tp") // 2
    place = lax.axis_index("tp")
    core = place % 2
    chip = place // 2
    index = lax.axis_index("ep")
    full_width = expert_gate.shape[1]

    def weight_for(expert):
        return jnp.sum(jnp.where(routes == expert, route_weights, 0.0), axis=1)[None, :]

    combine = [weight_for(index)] + [flip(weight_for(index ^ j), j) for j in range(1, 4)]
    combine = jnp.concatenate(combine, axis=1).reshape(4 * row_count, 1)

    def from_chip(step):
        if step == 0:
            return routed_input
        return lax.ppermute(routed_input, "tp", chip_shift(-step))

    def rows_of(weight, slot):
        return lax.dynamic_slice_in_dim(weight, slot * width, width, 0)

    def columns_of(weight, slot):
        return lax.dynamic_slice_in_dim(weight, slot * width, width, 1)

    def dot(left, right):
        return jnp.dot(left, right, preferred_element_type=jnp.float32)

    gate_sum = up_sum = square_sum = 0.0
    own_pieces = [None] * (2 * chips)
    for steps, relay in (((0,), 2), ((1, 3), 1), ((2,), 2)):
        steps = [step for step in steps if step < chips]
        if not steps:
            continue
        block = jnp.concatenate([from_chip(step) for step in steps], axis=1)
        held = jnp.concatenate(gather_square(block, relay), axis=0)
        swapped = lax.ppermute(held, "tp", cores_swap())
        for side, both in enumerate((held, swapped)):
            for at, step in enumerate(steps):
                values = both[:, at * width : (at + 1) * width]
                own_pieces[2 * step + side] = values[:row_count]
                slot = ((chip + step) % chips) * 2 + (core if side == 0 else 1 - core)
                gate_sum = gate_sum + dot(values, rows_of(expert_gate[0], slot))
                up_sum = up_sum + dot(values, rows_of(expert_up[0], slot))
                square_sum = square_sum + jnp.sum(
                    jnp.square(values.astype(jnp.float32)), axis=1, keepdims=True
                )
    stacked = jnp.stack(own_pieces)
    own_rows = jnp.concatenate(
        [
            lax.dynamic_index_in_dim(
                stacked,
                2 * ((z - chip) % chips) + (core if c == 0 else 1 - core),
                0,
                keepdims=False,
            )
            for z in range(chips)
            for c in range(2)
        ],
        axis=1,
    )

    def silu(v):
        return 0.5 * v * (1.0 + jnp.tanh(0.5 * v))

    factor = lax.rsqrt(square_sum / full_width + NORM_EPS)
    own_factor = factor[:row_count]
    shared_hidden = (
        silu(dot(own_rows, shared_gate) * own_factor) * (dot(own_rows, shared_up) * own_factor)
    ).astype(jnp.bfloat16)
    hidden = (silu(gate_sum * factor) * (up_sum * factor) * combine).astype(jnp.bfloat16)

    def partial(slot):
        down = columns_of(expert_down[0], slot)
        first = dot(hidden[:row_count], down) + dot(shared_hidden, columns_of(shared_down, slot))
        return first, dot(hidden[row_count:], down)

    total = 0.0
    for steps, relay in (((2, 1), 1), ((3, 0), 2)):
        steps = [step for step in steps if step < chips]
        slots = [((chip + step) % chips) * 2 for step in steps]
        leaving = []
        for slot in slots:
            first, rest = partial(slot + 1 - core)
            leaving.append(
                jnp.concatenate([first.astype(jnp.bfloat16), rest.astype(jnp.bfloat16)], axis=0)
            )
        arrived = lax.ppermute(jnp.concatenate(leaving, axis=1), "tp", cores_swap())
        sides = []
        for at, slot in enumerate(slots):
            first, rest = partial(slot + core)
            came = arrived[:, at * width : (at + 1) * width].astype(jnp.float32)
            sides.append(
                [first + came[:row_count]]
                + [
                    rest[j * row_count : (j + 1) * row_count]
                    + came[(j + 1) * row_count : (j + 2) * row_count]
                    for j in range(3)
                ]
            )
        result = scatter_square([jnp.concatenate(pair, axis=1) for pair in zip(*sides)], relay)
        for at, step in enumerate(steps):
            one = result[:, at * width : (at + 1) * width]
            if step:
                one = lax.ppermute(one.astype(jnp.bfloat16), "tp", chip_shift(step))
            total = total + one.astype(jnp.float32)
    return total.astype(jnp.bfloat16)


def body(
    query_heads,
    key_heads,
    value_heads,
    diff_lambda,
    sub_gain,
    out_weight,
    routed_input,
    routes,
    route_weights,
    expert_gate,
    expert_up,
    expert_down,
    shared_gate,
    shared_up,
    shared_down,
):
    groups = lax.axis_size("ep")
    local_experts = expert_gate.shape[0]
    capacity = 2 * routed_input.shape[0] * routes.shape[1] // (local_experts * groups)
    if (
        groups == 4
        and local_experts == 1
        and lax.axis_size("tp") in (4, 8)
        and capacity >= routed_input.shape[0]
    ):
        return (
            dense_mixer(query_heads, key_heads, value_heads, diff_lambda, sub_gain, out_weight),
            dense_experts(
                routed_input,
                routes,
                route_weights,
                expert_gate,
                expert_up,
                expert_down,
                shared_gate,
                shared_up,
                shared_down,
            ),
        )
    mixer_partial = mixer_terms(
        query_heads, key_heads, value_heads, diff_lambda, sub_gain, out_weight
    )
    routed_sum, shared_terms, placer = expert_terms(
        routed_input,
        routes,
        expert_gate,
        expert_up,
        expert_down,
        shared_gate,
        shared_up,
        shared_down,
    )
    mixer_sum, shared_sum = (
        lax.psum_scatter(
            mixer_partial.astype(jnp.bfloat16), "tp", scatter_dimension=1, tiled=True
        ).astype(jnp.float32),
        lax.psum_scatter(
            shared_terms.astype(jnp.bfloat16), "tp", scatter_dimension=1, tiled=True
        ).astype(jnp.float32),
    )
    return (
        mixer_sum.astype(jnp.bfloat16),
        expert_finish(routed_sum, shared_sum, placer, route_weights),
    )


def solution(mesh):
    placed = (
        P("ep", "tp"),
        P("ep", "tp"),
        P("ep", "tp"),
        P("tp"),
        P(),
        P("tp", None),
        P("ep", "tp"),
        P("ep", None),
        P("ep", None),
        P("ep", None, "tp"),
        P("ep", None, "tp"),
        P("ep", "tp", None),
        P(None, "tp"),
        P(None, "tp"),
        P("tp", None),
    )
    return jax.shard_map(
        body, mesh=mesh, in_specs=placed, out_specs=(P("ep", "tp"), P("ep", "tp")), check_vma=False
    )
```
